32 devices in a mesh: st: 8 (over z, x), tp: 4 (over y, core).
Axes of the slice: x: 2, y: 2, z: 4, core: 2. Of those that a mesh axis runs over, the one named last changes fastest.
Arguments:
- symbol_activations: bfloat16 [6144, 2048], P('st', 'tp'), may hold values from -6 to 6
- document_corpus: bfloat16 [128, 96, 2048], P('st'), may hold values from -6 to 6
- document_choice_matrix: int32 [48, 4], P('st'), may hold values from 0 to 127, as said below
- memory_probe_matrix: bfloat16 [2048, 1024], P(None, 'tp'), may hold values from -0.125 to 0.125
- memory_lookup_matrix: bfloat16 [2048, 1024], P(None, 'tp'), may hold values from -0.125 to 0.125
- memory_content_matrix: bfloat16 [2048, 1024], P(None, 'tp'), may hold values from -0.125 to 0.125
- valve_matrix: bfloat16 [2048, 16], replicated, may hold values from -0.125 to 0.125
- valve_biases: float32 [16], replicated, may hold values from -3 to 9
- added_decay_logit: float32 [6144, 8], P('st'), may hold values from -1 to 0
- facet_rescale_factor: float32 [1024], P('tp'), may hold values from 0.1 to 1.9
- document_probe_matrix: bfloat16 [2048, 1024], P(None, 'tp'), may hold values from -0.125 to 0.125
- document_lookup_matrix: bfloat16 [2048, 1024], P(None, 'tp'), may hold values from -0.125 to 0.125
- document_content_matrix: bfloat16 [2048, 1024], P(None, 'tp'), may hold values from -0.125 to 0.125
- document_rescale_factor: float32 [2048], replicated, may hold values from 0.1 to 1.9
- affinity_scaling: float32 [8], replicated, may hold values from 8 to 1200
- fetched_mixer_matrix: bfloat16 [2048, 1024], P(None, 'tp'), may hold values from -0.125 to 0.125
Outputs:
- mixed: bfloat16 [6144, 1024], P('st', 'tp')
The draws below stay inside these ranges and needn't reach their ends.
Inputs may be any that keep to these rules, and one draw needn't show every extreme that they name: `document_choice_matrix`: row b names the 4 passages that block b reads; passage p is held by index p // 16 of st. Among the rows of one sequence at most 6 ids name passages of one holder, and some holder is named exactly 6 times by each sequence.
All inputs are finite; a program needn't handle non-finite values.
Results may differ from the reference program's by a relative error of at most 0.0095.
The reference program's roundings to bfloat16 on the way count: a program that leaves them out, or rounds other values in their place, can miss the bound.
Values may be sent and summed in bfloat16 or wider, within the bound.
A program may use at most 128 MiB of HBM per device.

```python
import jax
import jax.numpy as jnp
from jax import lax

MODEL_WIDTH = 2048
FACET_COUNT = 8
LANE_DIMENSION = 128
STRING_LENGTH = 768
BLK = 128
SEG = 128
PASSAGE_READS = 4
PLEN = 96
P_DEV = 16
TOKENS = 6144
SEQUENCE_BLOCKS = 6
PASSAGES = 128
N_ST = 8


def draw_document_choice_matrix(key, part):
    request_count = STRING_LENGTH // BLK * PASSAGE_READS
    slot_cap = max(2, 2 * request_count // N_ST)
    slot_total = N_ST * slot_cap
    popular_key, device_key = jax.random.split(jax.random.fold_in(key, 11))
    popular = jax.random.randint(popular_key, (N_ST,), 0, 4)
    owner_of = jnp.arange(slot_total, dtype=jnp.int32) // slot_cap
    rank_in = jnp.arange(slot_total, dtype=jnp.int32) % slot_cap

    def one_device(device):
        sub_key = jax.random.fold_in(device_key, device)
        noise_key, shuffle_key, first_key, second_key = jax.random.split(sub_key, 4)
        score = jax.random.randint(noise_key, (slot_total,), 0, 65536) - popular[owner_of] * 65536
        before = (device + N_ST - 1) % N_ST
        across = (device + N_ST // 2) % N_ST
        score = jnp.where(owner_of == before, -(1 << 30), score)
        score = jnp.where((owner_of == across) & (rank_in == 0), -(1 << 29), score)
        chosen = jnp.argsort(score, stable=True)[:request_count]
        owners = owner_of[chosen][jax.random.permutation(shuffle_key, request_count)]
        within = jnp.minimum(jax.random.randint(first_key, (request_count,), 0, P_DEV), jax.random.randint(second_key, (request_count,), 0, P_DEV))
        return (owners * P_DEV + within).astype(jnp.int32)
    picked = jax.vmap(one_device)(jnp.arange(N_ST, dtype=jnp.int32))
    return picked.reshape(N_ST * request_count // PASSAGE_READS, PASSAGE_READS)


def draw_valve_biases(key, part):
    input_key, pick_key, noise_key = jax.random.split(jax.random.fold_in(key, 23), 3)
    input_rows = 0.5 * jax.random.normal(input_key, (FACET_COUNT,), jnp.float32)
    slow = jnp.log(jnp.float32(STRING_LENGTH))
    fast = jnp.log(jnp.float32(40.0))
    pick = jax.random.bernoulli(pick_key, 0.5, (FACET_COUNT,))
    forget = jnp.where(pick, slow, fast) + 0.3 * jax.random.normal(noise_key, (FACET_COUNT,), jnp.float32)
    return jnp.clip(jnp.concatenate([input_rows, forget]), -3.0, 9.0).astype(jnp.float32)


def draw_added_decay_logit(key, part):
    mask_key, depth_key = jax.random.split(jax.random.fold_in(key, 37))
    marked = jax.random.bernoulli(mask_key, 3.0 / STRING_LENGTH, (TOKENS, FACET_COUNT))
    depth = jnp.log(jax.random.uniform(depth_key, (TOKENS, FACET_COUNT), jnp.float32, 0.5, 0.8))
    return jnp.where(marked, depth, 0.0).astype(jnp.float32)


def draw_affinity_scaling(key, part):
    sub_key = jax.random.fold_in(key, 41)
    spread = jax.random.uniform(sub_key, (FACET_COUNT,), jnp.float32, jnp.log(8.0), jnp.log(24.0))
    return jnp.exp(spread).astype(jnp.float32)


def level_of(rng, extent, cuts, least, largest):
    factor_of, own = 1.0, jax.random.fold_in(rng, 6)
    for position, shards_of in cuts:
        draws = jnp.exp(jax.random.uniform(jax.random.fold_in(own, position), (shards_of,), jnp.float32, least / len(cuts), largest / len(cuts)))
        factor_of = factor_of * jnp.repeat(draws, extent[position] // shards_of).reshape([-1 if axis == position else 1 for axis in range(len(extent))])
    return factor_of


def centred(stream_key, dims, deviation, bound, pieces=(), kind=jnp.bfloat16):
    factor_of = level_of(stream_key, dims, pieces, -0.22, 0.18) if pieces else 1.0
    array = jax.random.normal(stream_key, dims, jnp.float32) * deviation * factor_of
    return jnp.minimum(jnp.maximum(array, -bound), bound).astype(kind)


def setup_inputs(seed: int = 0) -> dict:
    splits = jax.random.split(jax.random.key(seed), 17)
    symbol_activations = centred(splits[0], (TOKENS, MODEL_WIDTH), 1.0, 6.0, ((0, 8), (1, 4)))
    document_corpus = centred(splits[1], (PASSAGES, PLEN, MODEL_WIDTH), 1.0, 6.0, ((0, 8),))
    document_choice_matrix = draw_document_choice_matrix(jax.random.fold_in(splits[16], 71), 0)
    memory_probe_matrix = centred(splits[3], (MODEL_WIDTH, FACET_COUNT * LANE_DIMENSION), MODEL_WIDTH ** -0.5, 0.125, ((1, 4),))
    memory_lookup_matrix = centred(splits[4], (MODEL_WIDTH, FACET_COUNT * LANE_DIMENSION), MODEL_WIDTH ** -0.5, 0.125, ((1, 4),))
    memory_content_matrix = centred(splits[5], (MODEL_WIDTH, FACET_COUNT * LANE_DIMENSION), MODEL_WIDTH ** -0.5, 0.125, ((1, 4),))
    valve_matrix = centred(splits[6], (MODEL_WIDTH, 2 * FACET_COUNT), MODEL_WIDTH ** -0.5, 0.125)
    valve_biases = draw_valve_biases(jax.random.fold_in(splits[16], 71), 0)
    added_decay_logit = draw_added_decay_logit(jax.random.fold_in(splits[16], 71), 0)
    facet_rescale_factor = jnp.clip(1.0 + 0.18 * jax.random.normal(splits[9], (FACET_COUNT * LANE_DIMENSION,), jnp.float32), 0.1, 1.9)
    document_probe_matrix = centred(splits[10], (MODEL_WIDTH, FACET_COUNT * LANE_DIMENSION), MODEL_WIDTH ** -0.5, 0.125, ((1, 4),))
    document_lookup_matrix = centred(splits[11], (MODEL_WIDTH, FACET_COUNT * LANE_DIMENSION), MODEL_WIDTH ** -0.5, 0.125, ((1, 4),))
    document_content_matrix = centred(splits[12], (MODEL_WIDTH, FACET_COUNT * LANE_DIMENSION), MODEL_WIDTH ** -0.5, 0.125, ((1, 4),))
    document_rescale_factor = jnp.clip(1.0 + 0.18 * jax.random.normal(splits[13], (MODEL_WIDTH,), jnp.float32), 0.1, 1.9)
    affinity_scaling = draw_affinity_scaling(jax.random.fold_in(splits[16], 71), 0)
    fetched_mixer_matrix = centred(splits[15], (MODEL_WIDTH, FACET_COUNT * LANE_DIMENSION), MODEL_WIDTH ** -0.5, 0.125, ((1, 4),))
    return dict(symbol_activations=symbol_activations, document_corpus=document_corpus, document_choice_matrix=document_choice_matrix, memory_probe_matrix=memory_probe_matrix, memory_lookup_matrix=memory_lookup_matrix, memory_content_matrix=memory_content_matrix, valve_matrix=valve_matrix, valve_biases=valve_biases, added_decay_logit=added_decay_logit, facet_rescale_factor=facet_rescale_factor, document_probe_matrix=document_probe_matrix, document_lookup_matrix=document_lookup_matrix, document_content_matrix=document_content_matrix, document_rescale_factor=document_rescale_factor, affinity_scaling=affinity_scaling, fetched_mixer_matrix=fetched_mixer_matrix)


EPSILON = 1e-06
EMPTY_LOG = -1e+30
HIGHEST = lax.Precision.HIGHEST

def rms_scale(tensor):
    return lax.rsqrt(lax.optimization_barrier(jnp.mean(tensor * tensor, axis=-1, keepdims=True)) + EPSILON)

def cell_blocks(queries, key_rows, value_rows, input_logits, forget_log_gate):
    head_count, length, facet_dimension = queries.shape
    block_count = length // SEG

    def to_blocks(tensor):
        shaped = tensor.reshape((head_count, block_count, SEG) + tensor.shape[2:])
        return jnp.moveaxis(shaped, 1, 0)
    causal = jnp.tril(jnp.ones((SEG, SEG), dtype=bool))

    def advance(carry, blocks):
        memory, normal, stabilizer = carry
        query_part, key_part, value_part, input_part, forget_part = blocks
        cumulative = jnp.cumsum(forget_part, axis=-1)
        log_weight = jnp.where(causal, cumulative[:, :, None] - cumulative[:, None, :] + input_part[:, None, :], -jnp.inf)
        carried = cumulative + stabilizer[:, None]
        peak = jnp.maximum(carried, lax.optimization_barrier(jnp.max(log_weight, axis=-1)))
        weight = jnp.exp(log_weight - peak[:, :, None])
        old_weight = jnp.exp(carried - peak)
        affinity_logits = jnp.einsum('htd,hsd->hts', query_part, key_part, precision=HIGHEST) * weight
        numerator = old_weight[:, :, None] * jnp.einsum('htd,hde->hte', query_part, memory, precision=HIGHEST) + jnp.einsum('hts,hse->hte', affinity_logits, value_part, precision=HIGHEST)
        denominator = old_weight * jnp.einsum('htd,hd->ht', query_part, normal, precision=HIGHEST) + lax.optimization_barrier(jnp.sum(affinity_logits, axis=-1))
        final_output = numerator / jnp.maximum(jnp.abs(denominator), jnp.exp(-peak))[:, :, None]
        last_weight = weight[:, -1, :]
        old_last = old_weight[:, -1]
        weighted_keys = last_weight[:, :, None] * key_part
        memory = old_last[:, None, None] * memory + jnp.einsum('hsd,hse->hde', weighted_keys, value_part, precision=HIGHEST)
        normal = old_last[:, None] * normal + lax.optimization_barrier(jnp.sum(weighted_keys, axis=1))
        return ((memory, normal, peak[:, -1]), final_output)
    initial = (jnp.zeros((head_count, facet_dimension, facet_dimension), jnp.float32), jnp.zeros((head_count, facet_dimension), jnp.float32), jnp.full((head_count,), EMPTY_LOG, jnp.float32))
    scaled_keys = key_rows * facet_dimension ** (-0.5)
    final_state, outcome = lax.scan(advance, initial, (to_blocks(queries), to_blocks(scaled_keys), to_blocks(value_rows), to_blocks(input_logits), to_blocks(forget_log_gate)))
    return jnp.moveaxis(outcome, 0, 1).reshape(head_count, length, facet_dimension)

def document_lookup_update(probe_vectors, segment_lookups, segment_contents, facet_scales):
    facet_dimension = probe_vectors.shape[-1]
    affinity_logits = jnp.einsum('bqhd,bkhd->bhqk', probe_vectors.astype(jnp.float32), segment_lookups.astype(jnp.float32))
    ask_scale = rms_scale(probe_vectors.astype(jnp.float32))[..., 0]
    key_scale = rms_scale(segment_lookups.astype(jnp.float32))[..., 0]
    affinity_logits = affinity_logits * jnp.transpose(ask_scale, (0, 2, 1))[:, :, :, None]
    affinity_logits = affinity_logits * jnp.transpose(key_scale, (0, 2, 1))[:, :, None, :]
    affinity_logits = affinity_logits * (facet_scales / facet_dimension)[None, :, None, None]
    peak = lax.optimization_barrier(jnp.max(affinity_logits, axis=-1, keepdims=True))
    exp_scores = jnp.exp(affinity_logits - peak)
    weights = (exp_scores / lax.optimization_barrier(jnp.sum(exp_scores, axis=-1, keepdims=True))).astype(jnp.bfloat16)
    return jnp.einsum('bhqk,bkhd->bqhd', weights.astype(jnp.float32), segment_contents.astype(jnp.float32))

def reference(symbol_activations, document_corpus, document_choice_matrix, memory_probe_matrix, memory_lookup_matrix, memory_content_matrix, valve_matrix, valve_biases, added_decay_logit, facet_rescale_factor, document_probe_matrix, document_lookup_matrix, document_content_matrix, document_rescale_factor, affinity_scaling, fetched_mixer_matrix):
    store_rows = document_corpus.reshape(PASSAGES * PLEN, MODEL_WIDTH).astype(jnp.float32)
    normed = (store_rows * rms_scale(store_rows) * document_rescale_factor).astype(jnp.bfloat16)
    store_keys = jnp.dot(normed, document_lookup_matrix, preferred_element_type=jnp.float32).astype(jnp.bfloat16).reshape(PASSAGES, PLEN, FACET_COUNT * LANE_DIMENSION)
    store_values = jnp.dot(normed, document_content_matrix, preferred_element_type=jnp.float32).astype(jnp.bfloat16).reshape(PASSAGES, PLEN, FACET_COUNT * LANE_DIMENSION)

    def single_sequence(input_rows):
        sequence_token_rows, sequence_passage_index, sequence_extra_forget = input_rows

        def project(weight):
            return jnp.dot(sequence_token_rows, weight, preferred_element_type=jnp.float32)

        def heads_first(tensor):
            return jnp.transpose(tensor.astype(jnp.float32).reshape(STRING_LENGTH, FACET_COUNT, LANE_DIMENSION), (1, 0, 2))
        queries = project(memory_probe_matrix).astype(jnp.bfloat16)
        key_rows = project(memory_lookup_matrix).astype(jnp.bfloat16)
        value_rows = project(memory_content_matrix).astype(jnp.bfloat16)
        probe_vectors = project(document_probe_matrix).astype(jnp.bfloat16)
        mix_logits = project(fetched_mixer_matrix)
        gate_preactivation = project(valve_matrix) + valve_biases
        input_logits = gate_preactivation[:, :FACET_COUNT]
        forget_log_gate = jax.nn.log_sigmoid(gate_preactivation[:, FACET_COUNT:]) + sequence_extra_forget
        cell_out = cell_blocks(heads_first(queries), heads_first(key_rows), heads_first(value_rows), input_logits.T, forget_log_gate.T)
        cell_out = cell_out * rms_scale(cell_out) * facet_rescale_factor.reshape(FACET_COUNT, 1, LANE_DIMENSION)
        cell_out = jnp.transpose(cell_out, (1, 0, 2)).reshape(STRING_LENGTH, FACET_COUNT * LANE_DIMENSION)
        segment_lookups = store_keys[sequence_passage_index].reshape(SEQUENCE_BLOCKS, PASSAGE_READS * PLEN, FACET_COUNT, LANE_DIMENSION)
        segment_contents = store_values[sequence_passage_index].reshape(SEQUENCE_BLOCKS, PASSAGE_READS * PLEN, FACET_COUNT, LANE_DIMENSION)
        segment_probes = probe_vectors.reshape(SEQUENCE_BLOCKS, STRING_LENGTH // SEQUENCE_BLOCKS, FACET_COUNT, LANE_DIMENSION)
        fetched_result = document_lookup_update(segment_probes, segment_lookups, segment_contents, affinity_scaling).reshape(STRING_LENGTH, FACET_COUNT * LANE_DIMENSION)
        return (cell_out + jax.nn.sigmoid(mix_logits) * fetched_result).astype(jnp.bfloat16)
    final_output = lax.map(single_sequence, (symbol_activations.reshape(N_ST, STRING_LENGTH, MODEL_WIDTH), document_choice_matrix.reshape(N_ST, SEQUENCE_BLOCKS, PASSAGE_READS), added_decay_logit.reshape(N_ST, STRING_LENGTH, FACET_COUNT)))
    return final_output.reshape(TOKENS, FACET_COUNT * LANE_DIMENSION)
```

```python
import functools

import jax
import jax.numpy as jnp
from jax import lax
from jax.experimental import pallas as pl
from jax.experimental.pallas import tpu as pltpu
from jax.sharding import PartitionSpec as P

FACET_COUNT = 8
LANE_DIMENSION = 128
SEG = 128


EPSILON = 1e-06
EMPTY_LOG = -1e30
HIGHEST = lax.Precision.HIGHEST


def rms_scale(tensor):
    return lax.rsqrt(jnp.mean(tensor * tensor, axis=-1, keepdims=True) + EPSILON)


def cell_blocks(queries, key_rows, value_rows, input_logits, forget_log_gate):
    head_count, length, facet_dimension = queries.shape
    block_count = length // SEG

    def to_blocks(tensor):
        shaped = tensor.reshape((head_count, block_count, SEG) + tensor.shape[2:])
        return jnp.moveaxis(shaped, 1, 0)

    causal = jnp.tril(jnp.ones((SEG, SEG), dtype=bool))

    def advance(carry, blocks):
        memory, normal, stabilizer = carry
        query_part, key_part, value_part, input_part, forget_part = blocks
        cumulative = jnp.cumsum(forget_part, axis=-1)
        log_weight = jnp.where(
            causal,
            cumulative[:, :, None] - cumulative[:, None, :] + input_part[:, None, :],
            -jnp.inf,
        )
        carried = cumulative + stabilizer[:, None]
        peak = jnp.maximum(carried, jnp.max(log_weight, axis=-1))
        weight = jnp.exp(log_weight - peak[:, :, None])
        old_weight = jnp.exp(carried - peak)
        affinity_logits = (
            jnp.einsum("htd,hsd->hts", query_part, key_part, precision=HIGHEST) * weight
        )
        numerator = old_weight[:, :, None] * jnp.einsum(
            "htd,hde->hte", query_part, memory, precision=HIGHEST
        ) + jnp.einsum("hts,hse->hte", affinity_logits, value_part, precision=HIGHEST)
        denominator = old_weight * jnp.einsum(
            "htd,hd->ht", query_part, normal, precision=HIGHEST
        ) + jnp.sum(affinity_logits, axis=-1)
        final_output = numerator / jnp.maximum(jnp.abs(denominator), jnp.exp(-peak))[:, :, None]
        last_weight = weight[:, -1, :]
        old_last = old_weight[:, -1]
        weighted_keys = last_weight[:, :, None] * key_part
        memory = old_last[:, None, None] * memory + jnp.einsum(
            "hsd,hse->hde", weighted_keys, value_part, precision=HIGHEST
        )
        normal = old_last[:, None] * normal + jnp.sum(weighted_keys, axis=1)
        return ((memory, normal, peak[:, -1]), final_output)

    initial = (
        jnp.zeros((head_count, facet_dimension, facet_dimension), jnp.float32),
        jnp.zeros((head_count, facet_dimension), jnp.float32),
        jnp.full((head_count,), EMPTY_LOG, jnp.float32),
    )
    scaled_keys = key_rows * facet_dimension ** (-0.5)
    final_state, outcome = lax.scan(
        advance,
        initial,
        (
            to_blocks(queries),
            to_blocks(scaled_keys),
            to_blocks(value_rows),
            to_blocks(input_logits),
            to_blocks(forget_log_gate),
        ),
    )
    return jnp.moveaxis(outcome, 0, 1).reshape(head_count, length, facet_dimension)


def store_kernel(
    incoming, rows_ref, gain_ref, key_weight_ref, value_weight_ref, sent_ref, held, sems
):
    step = pl.program_id(0)
    per_step, row_count, width = rows_ref.shape
    half = key_weight_ref.shape[1]
    widened = rows_ref[...].reshape(per_step * row_count, width).astype(jnp.float32)
    normed = (widened * rms_scale(widened) * gain_ref[...]).astype(jnp.bfloat16)
    out_shape = (per_step, row_count, half)
    here = pl.ds(step * per_step, per_step)
    held[here, :, :half] = (
        jnp.dot(normed, key_weight_ref[...], preferred_element_type=jnp.float32)
        .astype(jnp.bfloat16)
        .reshape(out_shape)
    )
    held[here, :, half:] = (
        jnp.dot(normed, value_weight_ref[...], preferred_element_type=jnp.float32)
        .astype(jnp.bfloat16)
        .reshape(out_shape)
    )

    @pl.when(step == pl.num_programs(0) - 1)
    def _():
        slot_count = sent_ref.shape[0]

        def copy_of(slot):
            return pltpu.make_async_copy(
                held.at[incoming[slot]], sent_ref.at[slot], sems.at[slot]
            )

        def begin(slot, carry):
            copy_of(slot).start()
            return carry

        def finish(slot, carry):
            copy_of(slot).wait()
            return carry

        lax.fori_loop(0, slot_count, begin, 0)
        lax.fori_loop(0, slot_count, finish, 0)


def store_rows(
    incoming, document_corpus, document_rescale_factor, document_lookup_matrix, document_content_matrix
):
    passage_count, row_count, width = document_corpus.shape
    half = document_lookup_matrix.shape[1]
    slots = incoming.shape[0]
    per_step = 2
    whole = pl.BlockSpec((width, half), lambda i, ids: (0, 0))
    return pl.pallas_call(
        store_kernel,
        out_shape=jax.ShapeDtypeStruct((slots, row_count, 2 * half), jnp.bfloat16),
        grid_spec=pltpu.PrefetchScalarGridSpec(
            num_scalar_prefetch=1,
            grid=(passage_count // per_step,),
            in_specs=[
                pl.BlockSpec((per_step, row_count, width), lambda i, ids: (i, 0, 0)),
                pl.BlockSpec((1, width), lambda i, ids: (0, 0)),
                whole,
                whole,
            ],
            out_specs=pl.BlockSpec(memory_space=pl.ANY),
            scratch_shapes=[
                pltpu.VMEM((passage_count, row_count, 2 * half), jnp.bfloat16),
                pltpu.SemaphoreType.DMA((slots,)),
            ],
        ),
        compiler_params=pltpu.CompilerParams(dimension_semantics=("arbitrary",)),
        cost_estimate=pl.CostEstimate(
            flops=4 * passage_count * row_count * width * half,
            bytes_accessed=2 * passage_count * row_count * width,
            transcendentals=0,
        ),
    )(
        incoming,
        document_corpus,
        document_rescale_factor.reshape(1, width),
        document_lookup_matrix,
        document_content_matrix,
    )


TRANS = (((1,), (1,)), ((), ()))


def attend_kernel(reads, slot_ref, *refs):
    passages = refs[:reads]
    ask_ref, mix_ref, cell_ref, scale_ref, out_ref = refs[reads:]
    width = ask_ref.shape[1]
    facets = width // LANE_DIMENSION
    ones = jnp.full((8, LANE_DIMENSION), 1.0, jnp.float32)
    for facet in range(facets):
        lanes = slice(facet * LANE_DIMENSION, (facet + 1) * LANE_DIMENSION)
        value_lanes = slice(width + lanes.start, width + lanes.stop)
        ask = ask_ref[:, lanes]
        keys = jnp.concatenate([ref[0, :, lanes] for ref in passages], axis=0)
        values = jnp.concatenate([ref[0, :, value_lanes] for ref in passages], axis=0)
        wide_keys = keys.astype(jnp.float32)
        squares = lax.dot_general(
            ones, wide_keys * wide_keys, TRANS, precision=HIGHEST,
            preferred_element_type=jnp.float32,
        )
        key_scale = lax.rsqrt(squares[0:1] * (1.0 / LANE_DIMENSION) + EPSILON)
        ask_scale = rms_scale(ask.astype(jnp.float32))
        scores = lax.dot_general(ask, keys, TRANS, preferred_element_type=jnp.float32)
        scores = scores * ask_scale * key_scale * (scale_ref[0, facet] / LANE_DIMENSION)
        exp_scores = jnp.exp(scores - jnp.max(scores, axis=-1, keepdims=True))
        weights = (exp_scores / jnp.sum(exp_scores, axis=-1, keepdims=True)).astype(jnp.bfloat16)
        found = jnp.dot(weights, values, preferred_element_type=jnp.float32)
        out_ref[:, lanes] = (
            cell_ref[:, lanes] + jax.nn.sigmoid(mix_ref[:, lanes]) * found
        ).astype(jnp.bfloat16)


def attend(slot_index, slots, ask, mix_logits, cell_out, facet_scales, block_count):
    tok_rows, width = ask.shape
    reads = slot_index.shape[0] // block_count
    block_rows = tok_rows // block_count
    row_count = slots.shape[1]

    def passage_spec(place):
        return pl.BlockSpec(
            (1, row_count, slots.shape[2]), lambda b, ids: (ids[reads * b + place], 0, 0)
        )

    rows = pl.BlockSpec((block_rows, width), lambda b, ids: (b, 0))
    return pl.pallas_call(
        functools.partial(attend_kernel, reads),
        out_shape=jax.ShapeDtypeStruct((tok_rows, width), jnp.bfloat16),
        grid_spec=pltpu.PrefetchScalarGridSpec(
            num_scalar_prefetch=1,
            grid=(block_count,),
            in_specs=[passage_spec(place) for place in range(reads)]
            + [rows, rows, rows, pl.BlockSpec(memory_space=pltpu.SMEM)],
            out_specs=rows,
        ),
        compiler_params=pltpu.CompilerParams(dimension_semantics=("arbitrary",)),
        cost_estimate=pl.CostEstimate(
            flops=4 * tok_rows * reads * row_count * width,
            bytes_accessed=4 * slots.size,
            transcendentals=tok_rows * reads * row_count,
        ),
    )(
        slot_index,
        *([slots] * reads),
        ask,
        mix_logits,
        cell_out,
        facet_scales.reshape(1, -1),
    )


def local(
    symbol_activations,
    document_corpus,
    document_choice_matrix,
    memory_probe_matrix,
    memory_lookup_matrix,
    memory_content_matrix,
    valve_matrix,
    valve_biases,
    added_decay_logit,
    facet_rescale_factor,
    document_probe_matrix,
    document_lookup_matrix,
    document_content_matrix,
    document_rescale_factor,
    affinity_scaling,
    fetched_mixer_matrix,
):
    head_index = lax.axis_index("tp")
    local_width = memory_probe_matrix.shape[1]
    local_facets = local_width // LANE_DIMENSION
    tok_rows = symbol_activations.shape[0]
    joined = jnp.concatenate(
        [
            memory_probe_matrix,
            memory_lookup_matrix,
            memory_content_matrix,
            document_probe_matrix,
            fetched_mixer_matrix,
        ],
        axis=1,
    )
    token_piece = lax.all_gather(symbol_activations, "tp", axis=1, tiled=True)
    projected = jnp.dot(token_piece, joined, preferred_element_type=jnp.float32)
    gate_preactivation = jnp.dot(token_piece, valve_matrix, preferred_element_type=jnp.float32)
    queries = projected[:, :local_width].astype(jnp.bfloat16)
    key_rows = projected[:, local_width : 2 * local_width].astype(jnp.bfloat16)
    value_rows = projected[:, 2 * local_width : 3 * local_width].astype(jnp.bfloat16)
    probe_vectors = projected[:, 3 * local_width : 4 * local_width].astype(jnp.bfloat16)
    mix_logits = projected[:, 4 * local_width :]
    first_facet = head_index * local_facets
    gate_preactivation = gate_preactivation + valve_biases
    input_logits = lax.dynamic_slice_in_dim(gate_preactivation, first_facet, local_facets, 1)
    forget_logits = lax.dynamic_slice_in_dim(
        gate_preactivation, FACET_COUNT + first_facet, local_facets, 1
    )
    forget_log_gate = jax.nn.log_sigmoid(forget_logits) + lax.dynamic_slice_in_dim(
        added_decay_logit, first_facet, local_facets, 1
    )

    def heads_first(tensor):
        return jnp.transpose(
            tensor.astype(jnp.float32).reshape(tok_rows, local_facets, LANE_DIMENSION), (1, 0, 2)
        )

    cell_out = cell_blocks(
        heads_first(queries),
        heads_first(key_rows),
        heads_first(value_rows),
        input_logits.T,
        forget_log_gate.T,
    )
    cell_out = (
        cell_out
        * rms_scale(cell_out)
        * facet_rescale_factor.reshape(local_facets, 1, LANE_DIMENSION)
    )
    cell_out = jnp.transpose(cell_out, (1, 0, 2)).reshape(tok_rows, local_width)
    st_devices = lax.axis_size("st")
    flat_ids = document_choice_matrix.reshape(-1)
    request_count = flat_ids.shape[0]
    block_count = document_choice_matrix.shape[0]
    slot_cap = max(2, 2 * request_count // st_devices)
    per_owner = document_corpus.shape[0]
    owners = flat_ids // per_owner
    within = flat_ids % per_owner
    order_index = jnp.arange(request_count, dtype=jnp.int32)
    same_owner = (owners[:, None] == owners[None, :]) & (
        order_index[:, None] > order_index[None, :]
    )
    rank_among = jnp.sum(same_owner.astype(jnp.int32), axis=1)
    slot_index = owners * slot_cap + rank_among
    slot_hits = (
        slot_index[:, None] == jnp.arange(st_devices * slot_cap, dtype=jnp.int32)[None, :]
    ).astype(jnp.int32)
    outgoing = jnp.sum(slot_hits * within[:, None], axis=0).reshape(st_devices, slot_cap)
    incoming = lax.all_to_all(outgoing, "st", split_axis=0, concat_axis=0, tiled=True)
    outgoing_rows = store_rows(
        incoming.reshape(-1),
        document_corpus,
        document_rescale_factor,
        document_lookup_matrix,
        document_content_matrix,
    )
    slots = lax.all_to_all(outgoing_rows, "st", split_axis=0, concat_axis=0, tiled=True)
    facet_scales = lax.dynamic_slice_in_dim(affinity_scaling, first_facet, local_facets, 0)
    return attend(
        slot_index, slots, probe_vectors, mix_logits, cell_out, facet_scales, block_count
    )


def solution(mesh):
    return jax.shard_map(
        local,
        mesh=mesh,
        in_specs=(
            P("st", "tp"),
            P("st", None, None),
            P("st", None),
            P(None, "tp"),
            P(None, "tp"),
            P(None, "tp"),
            P(),
            P(),
            P("st", None),
            P("tp"),
            P(None, "tp"),
            P(None, "tp"),
            P(None, "tp"),
            P(),
            P(),
            P(None, "tp"),
        ),
        out_specs=P("st", "tp"),
        check_vma=False,
    )
```

```python
import functools

import jax
import jax.numpy as jnp
from jax import lax
from jax.experimental import pallas as pl
from jax.experimental.pallas import tpu as pltpu
from jax.sharding import PartitionSpec as P

FACET_COUNT = 8
LANE_DIMENSION = 128
SEG = 128


EPSILON = 1e-06
EMPTY_LOG = -1e30
HIGHEST = lax.Precision.HIGHEST


def rms_scale(tensor):
    return lax.rsqrt(jnp.mean(tensor * tensor, axis=-1, keepdims=True) + EPSILON)


def cell_blocks(queries, key_rows, value_rows, input_logits, forget_log_gate):
    head_count, length, facet_dimension = queries.shape
    block_count = length // SEG

    def to_blocks(tensor):
        shaped = tensor.reshape((head_count, block_count, SEG) + tensor.shape[2:])
        return jnp.moveaxis(shaped, 1, 0)

    causal = jnp.tril(jnp.ones((SEG, SEG), dtype=bool))

    def advance(carry, blocks):
        memory, normal, stabilizer = carry
        query_part, key_part, value_part, input_part, forget_part = blocks
        cumulative = jnp.cumsum(forget_part, axis=-1)
        log_weight = jnp.where(
            causal,
            cumulative[:, :, None] - cumulative[:, None, :] + input_part[:, None, :],
            -jnp.inf,
        )
        carried = cumulative + stabilizer[:, None]
        peak = jnp.maximum(carried, jnp.max(log_weight, axis=-1))
        weight = jnp.exp(log_weight - peak[:, :, None])
        old_weight = jnp.exp(carried - peak)
        affinity_logits = (
            jnp.einsum("htd,hsd->hts", query_part, key_part, precision=HIGHEST) * weight
        )
        numerator = old_weight[:, :, None] * jnp.einsum(
            "htd,hde->hte", query_part, memory, precision=HIGHEST
        ) + jnp.einsum("hts,hse->hte", affinity_logits, value_part, precision=HIGHEST)
        denominator = old_weight * jnp.einsum(
            "htd,hd->ht", query_part, normal, precision=HIGHEST
        ) + jnp.sum(affinity_logits, axis=-1)
        final_output = numerator / jnp.maximum(jnp.abs(denominator), jnp.exp(-peak))[:, :, None]
        last_weight = weight[:, -1, :]
        old_last = old_weight[:, -1]
        weighted_keys = last_weight[:, :, None] * key_part
        memory = old_last[:, None, None] * memory + jnp.einsum(
            "hsd,hse->hde", weighted_keys, value_part, precision=HIGHEST
        )
        normal = old_last[:, None] * normal + jnp.sum(weighted_keys, axis=1)
        return ((memory, normal, peak[:, -1]), final_output)

    initial = (
        jnp.zeros((head_count, facet_dimension, facet_dimension), jnp.float32),
        jnp.zeros((head_count, facet_dimension), jnp.float32),
        jnp.full((head_count,), EMPTY_LOG, jnp.float32),
    )
    scaled_keys = key_rows * facet_dimension ** (-0.5)
    final_state, outcome = lax.scan(
        advance,
        initial,
        (
            to_blocks(queries),
            to_blocks(scaled_keys),
            to_blocks(value_rows),
            to_blocks(input_logits),
            to_blocks(forget_log_gate),
        ),
    )
    return jnp.moveaxis(outcome, 0, 1).reshape(head_count, length, facet_dimension)


def store_kernel(
    incoming, rows_ref, gain_ref, key_weight_ref, value_weight_ref, sent_ref, held, sems
):
    step = pl.program_id(0)
    per_step, row_count, width = rows_ref.shape
    half = key_weight_ref.shape[1]
    widened = rows_ref[...].reshape(per_step * row_count, width).astype(jnp.float32)
    normed = (widened * rms_scale(widened) * gain_ref[...]).astype(jnp.bfloat16)
    out_shape = (per_step, row_count, half)
    here = pl.ds(step * per_step, per_step)
    held[here, :, :half] = (
        jnp.dot(normed, key_weight_ref[...], preferred_element_type=jnp.float32)
        .astype(jnp.bfloat16)
        .reshape(out_shape)
    )
    held[here, :, half:] = (
        jnp.dot(normed, value_weight_ref[...], preferred_element_type=jnp.float32)
        .astype(jnp.bfloat16)
        .reshape(out_shape)
    )

    @pl.when(step == pl.num_programs(0) - 1)
    def _():
        slot_count = sent_ref.shape[0]

        def copy_of(slot):
            return pltpu.make_async_copy(
                held.at[incoming[slot]], sent_ref.at[slot], sems.at[slot]
            )

        def begin(slot, carry):
            copy_of(slot).start()
            return carry

        def finish(slot, carry):
            copy_of(slot).wait()
            return carry

        lax.fori_loop(0, slot_count, begin, 0)
        lax.fori_loop(0, slot_count, finish, 0)


def store_rows(
    incoming, document_corpus, document_rescale_factor, document_lookup_matrix, document_content_matrix
):
    passage_count, row_count, width = document_corpus.shape
    half = document_lookup_matrix.shape[1]
    slots = incoming.shape[0]
    per_step = 2
    whole = pl.BlockSpec((width, half), lambda i, ids: (0, 0))
    return pl.pallas_call(
        store_kernel,
        out_shape=jax.ShapeDtypeStruct((slots, row_count, 2 * half), jnp.bfloat16),
        grid_spec=pltpu.PrefetchScalarGridSpec(
            num_scalar_prefetch=1,
            grid=(passage_count // per_step,),
            in_specs=[
                pl.BlockSpec((per_step, row_count, width), lambda i, ids: (i, 0, 0)),
                pl.BlockSpec((1, width), lambda i, ids: (0, 0)),
                whole,
                whole,
            ],
            out_specs=pl.BlockSpec(memory_space=pl.ANY),
            scratch_shapes=[
                pltpu.VMEM((passage_count, row_count, 2 * half), jnp.bfloat16),
                pltpu.SemaphoreType.DMA((slots,)),
            ],
        ),
        compiler_params=pltpu.CompilerParams(dimension_semantics=("arbitrary",)),
        cost_estimate=pl.CostEstimate(
            flops=4 * passage_count * row_count * width * half,
            bytes_accessed=2 * passage_count * row_count * width,
            transcendentals=0,
        ),
    )(
        incoming,
        document_corpus,
        document_rescale_factor.reshape(1, width),
        document_lookup_matrix,
        document_content_matrix,
    )


TRANS = (((1,), (1,)), ((), ()))


def attend_kernel(reads, slot_ref, *refs):
    passages = refs[:reads]
    ask_ref, mix_ref, cell_ref, scale_ref, out_ref = refs[reads:]
    width = ask_ref.shape[1]
    facets = width // LANE_DIMENSION
    ones = jnp.full((8, LANE_DIMENSION), 1.0, jnp.bfloat16)
    for facet in range(facets):
        lanes = slice(facet * LANE_DIMENSION, (facet + 1) * LANE_DIMENSION)
        value_lanes = slice(width + lanes.start, width + lanes.stop)
        ask = ask_ref[:, lanes]
        keys = jnp.concatenate([ref[0, :, lanes] for ref in passages], axis=0)
        values = jnp.concatenate([ref[0, :, value_lanes] for ref in passages], axis=0)
        wide_keys = keys.astype(jnp.float32)
        squared = wide_keys * wide_keys
        high = squared.astype(jnp.bfloat16)
        low = (squared - high.astype(jnp.float32)).astype(jnp.bfloat16)
        squares = lax.dot_general(
            ones, high, TRANS, preferred_element_type=jnp.float32
        ) + lax.dot_general(ones, low, TRANS, preferred_element_type=jnp.float32)
        key_scale = lax.rsqrt(squares[0:1] * (1.0 / LANE_DIMENSION) + EPSILON)
        ask_scale = rms_scale(ask.astype(jnp.float32))
        scores = lax.dot_general(ask, keys, TRANS, preferred_element_type=jnp.float32)
        scores = scores * ask_scale * key_scale * (scale_ref[0, facet] / LANE_DIMENSION)
        exp_scores = jnp.exp(scores - jnp.max(scores, axis=-1, keepdims=True))
        weights = (exp_scores / jnp.sum(exp_scores, axis=-1, keepdims=True)).astype(jnp.bfloat16)
        found = jnp.dot(weights, values, preferred_element_type=jnp.float32)
        out_ref[:, lanes] = (
            cell_ref[:, lanes] + jax.nn.sigmoid(mix_ref[:, lanes]) * found
        ).astype(jnp.bfloat16)


def attend(slot_index, slots, ask, mix_logits, cell_out, facet_scales, block_count):
    tok_rows, width = ask.shape
    reads = slot_index.shape[0] // block_count
    block_rows = tok_rows // block_count
    row_count = slots.shape[1]

    def passage_spec(place):
        return pl.BlockSpec(
            (1, row_count, slots.shape[2]), lambda b, ids: (ids[reads * b + place], 0, 0)
        )

    rows = pl.BlockSpec((block_rows, width), lambda b, ids: (b, 0))
    return pl.pallas_call(
        functools.partial(attend_kernel, reads),
        out_shape=jax.ShapeDtypeStruct((tok_rows, width), jnp.bfloat16),
        grid_spec=pltpu.PrefetchScalarGridSpec(
            num_scalar_prefetch=1,
            grid=(block_count,),
            in_specs=[passage_spec(place) for place in range(reads)]
            + [rows, rows, rows, pl.BlockSpec(memory_space=pltpu.SMEM)],
            out_specs=rows,
        ),
        compiler_params=pltpu.CompilerParams(dimension_semantics=("arbitrary",)),
        cost_estimate=pl.CostEstimate(
            flops=4 * tok_rows * reads * row_count * width,
            bytes_accessed=4 * slots.size,
            transcendentals=tok_rows * reads * row_count,
        ),
    )(
        slot_index,
        *([slots] * reads),
        ask,
        mix_logits,
        cell_out,
        facet_scales.reshape(1, -1),
    )


def gather_features(piece):
    count = lax.axis_size("tp")
    me = lax.axis_index("tp")
    pieces = [piece]
    for shift in range(1, count):
        pairs = [((i + shift) % count, i) for i in range(count)]
        pieces.append(lax.ppermute(piece, "tp", pairs))
    stacked = jnp.stack(pieces)
    ordered = [
        lax.dynamic_index_in_dim(stacked, lax.rem(i - me + count, count), 0, keepdims=False)
        for i in range(count)
    ]
    return jnp.concatenate(ordered, axis=1)


def local(
    symbol_activations,
    document_corpus,
    document_choice_matrix,
    memory_probe_matrix,
    memory_lookup_matrix,
    memory_content_matrix,
    valve_matrix,
    valve_biases,
    added_decay_logit,
    facet_rescale_factor,
    document_probe_matrix,
    document_lookup_matrix,
    document_content_matrix,
    document_rescale_factor,
    affinity_scaling,
    fetched_mixer_matrix,
):
    head_index = lax.axis_index("tp")
    local_width = memory_probe_matrix.shape[1]
    local_facets = local_width // LANE_DIMENSION
    tok_rows = symbol_activations.shape[0]
    st_devices = lax.axis_size("st")
    flat_ids = document_choice_matrix.reshape(-1)
    request_count = flat_ids.shape[0]
    block_count = document_choice_matrix.shape[0]
    slot_cap = max(2, 2 * request_count // st_devices)
    per_owner = document_corpus.shape[0]
    owners = flat_ids // per_owner
    within = flat_ids % per_owner
    order_index = jnp.arange(request_count, dtype=jnp.int32)
    same_owner = (owners[:, None] == owners[None, :]) & (
        order_index[:, None] > order_index[None, :]
    )
    rank_among = jnp.sum(same_owner.astype(jnp.int32), axis=1)
    slot_index = owners * slot_cap + rank_among
    slot_hits = (
        slot_index[:, None] == jnp.arange(st_devices * slot_cap, dtype=jnp.int32)[None, :]
    ).astype(jnp.int32)
    outgoing = jnp.sum(slot_hits * within[:, None], axis=0).reshape(st_devices, slot_cap)
    incoming = lax.all_to_all(outgoing, "st", split_axis=0, concat_axis=0, tiled=True)
    outgoing_rows = store_rows(
        incoming.reshape(-1),
        document_corpus,
        document_rescale_factor,
        document_lookup_matrix,
        document_content_matrix,
    )
    (
        outgoing_rows,
        symbol_activations,
        memory_probe_matrix,
        memory_lookup_matrix,
        memory_content_matrix,
        document_probe_matrix,
        fetched_mixer_matrix,
    ) = lax.optimization_barrier(
        (
            outgoing_rows,
            symbol_activations,
            memory_probe_matrix,
            memory_lookup_matrix,
            memory_content_matrix,
            document_probe_matrix,
            fetched_mixer_matrix,
        )
    )
    joined = jnp.concatenate(
        [
            memory_probe_matrix,
            memory_lookup_matrix,
            memory_content_matrix,
            document_probe_matrix,
            fetched_mixer_matrix,
        ],
        axis=1,
    )
    token_piece = gather_features(symbol_activations)
    projected = jnp.dot(token_piece, joined, preferred_element_type=jnp.float32)
    gate_preactivation = jnp.dot(token_piece, valve_matrix, preferred_element_type=jnp.float32)
    queries = projected[:, :local_width].astype(jnp.bfloat16)
    key_rows = projected[:, local_width : 2 * local_width].astype(jnp.bfloat16)
    value_rows = projected[:, 2 * local_width : 3 * local_width].astype(jnp.bfloat16)
    probe_vectors = projected[:, 3 * local_width : 4 * local_width].astype(jnp.bfloat16)
    mix_logits = projected[:, 4 * local_width :]
    first_facet = head_index * local_facets
    gate_preactivation = gate_preactivation + valve_biases
    input_logits = lax.dynamic_slice_in_dim(gate_preactivation, first_facet, local_facets, 1)
    forget_logits = lax.dynamic_slice_in_dim(
        gate_preactivation, FACET_COUNT + first_facet, local_facets, 1
    )
    forget_log_gate = jax.nn.log_sigmoid(forget_logits) + lax.dynamic_slice_in_dim(
        added_decay_logit, first_facet, local_facets, 1
    )

    def heads_first(tensor):
        return jnp.transpose(
            tensor.astype(jnp.float32).reshape(tok_rows, local_facets, LANE_DIMENSION), (1, 0, 2)
        )

    cell_out = cell_blocks(
        heads_first(queries),
        heads_first(key_rows),
        heads_first(value_rows),
        input_logits.T,
        forget_log_gate.T,
    )
    cell_out = (
        cell_out
        * rms_scale(cell_out)
        * facet_rescale_factor.reshape(local_facets, 1, LANE_DIMENSION)
    )
    cell_out = jnp.transpose(cell_out, (1, 0, 2)).reshape(tok_rows, local_width)
    slots = lax.all_to_all(outgoing_rows, "st", split_axis=0, concat_axis=0, tiled=True)
    facet_scales = lax.dynamic_slice_in_dim(affinity_scaling, first_facet, local_facets, 0)
    return attend(
        slot_index, slots, probe_vectors, mix_logits, cell_out, facet_scales, block_count
    )


def solution(mesh):
    return jax.shard_map(
        local,
        mesh=mesh,
        in_specs=(
            P("st", "tp"),
            P("st", None, None),
            P("st", None),
            P(None, "tp"),
            P(None, "tp"),
            P(None, "tp"),
            P(),
            P(),
            P("st", None),
            P("tp"),
            P(None, "tp"),
            P(None, "tp"),
            P(None, "tp"),
            P(),
            P(),
            P(None, "tp"),
        ),
        out_specs=P("st", "tp"),
        check_vma=False,
    )
```

```python
import functools

import jax
import jax.numpy as jnp
from jax import lax
from jax.experimental import pallas as pl
from jax.experimental.pallas import tpu as pltpu
from jax.sharding import PartitionSpec as P

FACET_COUNT = 8
LANE_DIMENSION = 128
SEG = 128


EPSILON = 1e-06
EMPTY_LOG = -1e30
HIGHEST = lax.Precision.HIGHEST


def rms_scale(tensor):
    return lax.rsqrt(jnp.mean(tensor * tensor, axis=-1, keepdims=True) + EPSILON)


def cell_blocks(queries, key_rows, value_rows, input_logits, forget_log_gate):
    head_count, length, facet_dimension = queries.shape
    block_count = length // SEG

    def to_blocks(tensor):
        shaped = tensor.reshape((head_count, block_count, SEG) + tensor.shape[2:])
        return jnp.moveaxis(shaped, 1, 0)

    causal = jnp.tril(jnp.ones((SEG, SEG), dtype=bool))

    def advance(carry, blocks):
        memory, normal, stabilizer = carry
        query_part, key_part, value_part, input_part, forget_part = blocks
        cumulative = jnp.cumsum(forget_part, axis=-1)
        log_weight = jnp.where(
            causal,
            cumulative[:, :, None] - cumulative[:, None, :] + input_part[:, None, :],
            -jnp.inf,
        )
        carried = cumulative + stabilizer[:, None]
        peak = jnp.maximum(carried, jnp.max(log_weight, axis=-1))
        weight = jnp.exp(log_weight - peak[:, :, None])
        old_weight = jnp.exp(carried - peak)
        affinity_logits = (
            jnp.einsum("htd,hsd->hts", query_part, key_part, precision=HIGHEST) * weight
        )
        numerator = old_weight[:, :, None] * jnp.einsum(
            "htd,hde->hte", query_part, memory, precision=HIGHEST
        ) + jnp.einsum("hts,hse->hte", affinity_logits, value_part, precision=HIGHEST)
        denominator = old_weight * jnp.einsum(
            "htd,hd->ht", query_part, normal, precision=HIGHEST
        ) + jnp.sum(affinity_logits, axis=-1)
        final_output = numerator / jnp.maximum(jnp.abs(denominator), jnp.exp(-peak))[:, :, None]
        last_weight = weight[:, -1, :]
        old_last = old_weight[:, -1]
        weighted_keys = last_weight[:, :, None] * key_part
        memory = old_last[:, None, None] * memory + jnp.einsum(
            "hsd,hse->hde", weighted_keys, value_part, precision=HIGHEST
        )
        normal = old_last[:, None] * normal + jnp.sum(weighted_keys, axis=1)
        return ((memory, normal, peak[:, -1]), final_output)

    initial = (
        jnp.zeros((head_count, facet_dimension, facet_dimension), jnp.float32),
        jnp.zeros((head_count, facet_dimension), jnp.float32),
        jnp.full((head_count,), EMPTY_LOG, jnp.float32),
    )
    scaled_keys = key_rows * facet_dimension ** (-0.5)
    final_state, outcome = lax.scan(
        advance,
        initial,
        (
            to_blocks(queries),
            to_blocks(scaled_keys),
            to_blocks(value_rows),
            to_blocks(input_logits),
            to_blocks(forget_log_gate),
        ),
    )
    return jnp.moveaxis(outcome, 0, 1).reshape(head_count, length, facet_dimension)


def store_kernel(rows_ref, gain_ref, key_weight_ref, value_weight_ref, out_ref):
    per_step, row_count, width = rows_ref.shape
    half = key_weight_ref.shape[1]
    widened = rows_ref[...].reshape(per_step * row_count, width).astype(jnp.float32)
    normed = (widened * rms_scale(widened) * gain_ref[...]).astype(jnp.bfloat16)
    out_shape = (per_step, row_count, half)
    out_ref[:, :, :half] = (
        jnp.dot(normed, key_weight_ref[...], preferred_element_type=jnp.float32)
        .astype(jnp.bfloat16)
        .reshape(out_shape)
    )
    out_ref[:, :, half:] = (
        jnp.dot(normed, value_weight_ref[...], preferred_element_type=jnp.float32)
        .astype(jnp.bfloat16)
        .reshape(out_shape)
    )


def store_rows(
    document_corpus, document_rescale_factor, document_lookup_matrix, document_content_matrix
):
    passage_count, row_count, width = document_corpus.shape
    half = document_lookup_matrix.shape[1]
    per_step = 2
    whole = pl.BlockSpec((width, half), lambda i: (0, 0))
    return pl.pallas_call(
        store_kernel,
        out_shape=jax.ShapeDtypeStruct((passage_count, row_count, 2 * half), jnp.bfloat16),
        grid=(passage_count // per_step,),
        in_specs=[
            pl.BlockSpec((per_step, row_count, width), lambda i: (i, 0, 0)),
            pl.BlockSpec((1, width), lambda i: (0, 0)),
            whole,
            whole,
        ],
        out_specs=pl.BlockSpec((per_step, row_count, 2 * half), lambda i: (i, 0, 0)),
        compiler_params=pltpu.CompilerParams(dimension_semantics=("arbitrary",)),
        cost_estimate=pl.CostEstimate(
            flops=4 * passage_count * row_count * width * half,
            bytes_accessed=2 * passage_count * row_count * width,
            transcendentals=0,
        ),
    )(
        document_corpus,
        document_rescale_factor.reshape(1, width),
        document_lookup_matrix,
        document_content_matrix,
    )


def pick_kernel(incoming, held, sent_ref, sems):
    slot_count = sent_ref.shape[0]

    def copy_of(slot):
        return pltpu.make_async_copy(
            held.at[incoming[slot]], sent_ref.at[slot], sems.at[slot]
        )

    def begin(slot, carry):
        copy_of(slot).start()
        return carry

    def finish(slot, carry):
        copy_of(slot).wait()
        return carry

    lax.fori_loop(0, slot_count, begin, 0)
    lax.fori_loop(0, slot_count, finish, 0)


def pick_rows(incoming, store):
    slots = incoming.shape[0]
    shape = (slots,) + store.shape[1:]
    return pl.pallas_call(
        pick_kernel,
        out_shape=jax.ShapeDtypeStruct(shape, store.dtype),
        in_specs=[
            pl.BlockSpec(memory_space=pltpu.SMEM),
            pl.BlockSpec(memory_space=pltpu.VMEM),
        ],
        out_specs=pl.BlockSpec(memory_space=pl.ANY),
        scratch_shapes=[pltpu.SemaphoreType.DMA((slots,))],
    )(incoming, store)


TRANS = (((1,), (1,)), ((), ()))


def attend_kernel(reads, slot_ref, *refs):
    passages = refs[:reads]
    ask_ref, mix_ref, cell_ref, scale_ref, out_ref = refs[reads:]
    width = ask_ref.shape[1]
    facets = width // LANE_DIMENSION
    ones = jnp.full((8, LANE_DIMENSION), 1.0, jnp.bfloat16)
    for facet in range(facets):
        lanes = slice(facet * LANE_DIMENSION, (facet + 1) * LANE_DIMENSION)
        value_lanes = slice(width + lanes.start, width + lanes.stop)
        ask = ask_ref[:, lanes]
        keys = jnp.concatenate([ref[0, :, lanes] for ref in passages], axis=0)
        values = jnp.concatenate([ref[0, :, value_lanes] for ref in passages], axis=0)
        wide_keys = keys.astype(jnp.float32)
        squared = wide_keys * wide_keys
        high = squared.astype(jnp.bfloat16)
        low = (squared - high.astype(jnp.float32)).astype(jnp.bfloat16)
        squares = lax.dot_general(
            ones, high, TRANS, preferred_element_type=jnp.float32
        ) + lax.dot_general(ones, low, TRANS, preferred_element_type=jnp.float32)
        key_scale = lax.rsqrt(squares[0:1] * (1.0 / LANE_DIMENSION) + EPSILON)
        ask_scale = rms_scale(ask.astype(jnp.float32))
        scores = lax.dot_general(ask, keys, TRANS, preferred_element_type=jnp.float32)
        scores = scores * ask_scale * key_scale * (scale_ref[0, facet] / LANE_DIMENSION)
        exp_scores = jnp.exp(scores - jnp.max(scores, axis=-1, keepdims=True))
        weights = (exp_scores / jnp.sum(exp_scores, axis=-1, keepdims=True)).astype(jnp.bfloat16)
        found = jnp.dot(weights, values, preferred_element_type=jnp.float32)
        out_ref[:, lanes] = (
            cell_ref[:, lanes] + jax.nn.sigmoid(mix_ref[:, lanes]) * found
        ).astype(jnp.bfloat16)


def attend(slot_index, slots, ask, mix_logits, cell_out, facet_scales, block_count):
    tok_rows, width = ask.shape
    reads = slot_index.shape[0] // block_count
    block_rows = tok_rows // block_count
    row_count = slots.shape[1]

    def passage_spec(place):
        return pl.BlockSpec(
            (1, row_count, slots.shape[2]), lambda b, ids: (ids[reads * b + place], 0, 0)
        )

    rows = pl.BlockSpec((block_rows, width), lambda b, ids: (b, 0))
    return pl.pallas_call(
        functools.partial(attend_kernel, reads),
        out_shape=jax.ShapeDtypeStruct((tok_rows, width), jnp.bfloat16),
        grid_spec=pltpu.PrefetchScalarGridSpec(
            num_scalar_prefetch=1,
            grid=(block_count,),
            in_specs=[passage_spec(place) for place in range(reads)]
            + [rows, rows, rows, pl.BlockSpec(memory_space=pltpu.SMEM)],
            out_specs=rows,
        ),
        compiler_params=pltpu.CompilerParams(dimension_semantics=("arbitrary",)),
        cost_estimate=pl.CostEstimate(
            flops=4 * tok_rows * reads * row_count * width,
            bytes_accessed=4 * slots.size,
            transcendentals=tok_rows * reads * row_count,
        ),
    )(
        slot_index,
        *([slots] * reads),
        ask,
        mix_logits,
        cell_out,
        facet_scales.reshape(1, -1),
    )


def gather_features(piece):
    count = lax.axis_size("tp")
    me = lax.axis_index("tp")
    pieces = [piece]
    for shift in range(1, count):
        pairs = [((i + shift) % count, i) for i in range(count)]
        pieces.append(lax.ppermute(piece, "tp", pairs))
    stacked = jnp.stack(pieces)
    ordered = [
        lax.dynamic_index_in_dim(stacked, lax.rem(i - me + count, count), 0, keepdims=False)
        for i in range(count)
    ]
    return jnp.concatenate(ordered, axis=1)


def local(
    symbol_activations,
    document_corpus,
    document_choice_matrix,
    memory_probe_matrix,
    memory_lookup_matrix,
    memory_content_matrix,
    valve_matrix,
    valve_biases,
    added_decay_logit,
    facet_rescale_factor,
    document_probe_matrix,
    document_lookup_matrix,
    document_content_matrix,
    document_rescale_factor,
    affinity_scaling,
    fetched_mixer_matrix,
):
    head_index = lax.axis_index("tp")
    local_width = memory_probe_matrix.shape[1]
    local_facets = local_width // LANE_DIMENSION
    tok_rows = symbol_activations.shape[0]
    st_devices = lax.axis_size("st")
    flat_ids = document_choice_matrix.reshape(-1)
    request_count = flat_ids.shape[0]
    block_count = document_choice_matrix.shape[0]
    slot_cap = max(2, 2 * request_count // st_devices)
    per_owner = document_corpus.shape[0]
    owners = flat_ids // per_owner
    within = flat_ids % per_owner
    order_index = jnp.arange(request_count, dtype=jnp.int32)
    same_owner = (owners[:, None] == owners[None, :]) & (
        order_index[:, None] > order_index[None, :]
    )
    rank_among = jnp.sum(same_owner.astype(jnp.int32), axis=1)
    slot_index = owners * slot_cap + rank_among
    slot_hits = (
        slot_index[:, None] == jnp.arange(st_devices * slot_cap, dtype=jnp.int32)[None, :]
    ).astype(jnp.int32)
    outgoing = jnp.sum(slot_hits * within[:, None], axis=0).reshape(st_devices, slot_cap)
    incoming = lax.all_to_all(outgoing, "st", split_axis=0, concat_axis=0, tiled=True)
    store = store_rows(
        document_corpus,
        document_rescale_factor,
        document_lookup_matrix,
        document_content_matrix,
    )
    outgoing_rows = pick_rows(incoming.reshape(-1), store)
    (
        outgoing_rows,
        symbol_activations,
        memory_probe_matrix,
        memory_lookup_matrix,
        memory_content_matrix,
        document_probe_matrix,
        fetched_mixer_matrix,
    ) = lax.optimization_barrier(
        (
            outgoing_rows,
            symbol_activations,
            memory_probe_matrix,
            memory_lookup_matrix,
            memory_content_matrix,
            document_probe_matrix,
            fetched_mixer_matrix,
        )
    )
    joined = jnp.concatenate(
        [
            memory_probe_matrix,
            memory_lookup_matrix,
            memory_content_matrix,
            document_probe_matrix,
            fetched_mixer_matrix,
        ],
        axis=1,
    )
    token_piece = gather_features(symbol_activations)
    projected = jnp.dot(token_piece, joined, preferred_element_type=jnp.float32)
    gate_preactivation = jnp.dot(token_piece, valve_matrix, preferred_element_type=jnp.float32)
    queries = projected[:, :local_width].astype(jnp.bfloat16)
    key_rows = projected[:, local_width : 2 * local_width].astype(jnp.bfloat16)
    value_rows = projected[:, 2 * local_width : 3 * local_width].astype(jnp.bfloat16)
    probe_vectors = projected[:, 3 * local_width : 4 * local_width].astype(jnp.bfloat16)
    mix_logits = projected[:, 4 * local_width :]
    first_facet = head_index * local_facets
    gate_preactivation = gate_preactivation + valve_biases
    input_logits = lax.dynamic_slice_in_dim(gate_preactivation, first_facet, local_facets, 1)
    forget_logits = lax.dynamic_slice_in_dim(
        gate_preactivation, FACET_COUNT + first_facet, local_facets, 1
    )
    forget_log_gate = jax.nn.log_sigmoid(forget_logits) + lax.dynamic_slice_in_dim(
        added_decay_logit, first_facet, local_facets, 1
    )

    def heads_first(tensor):
        return jnp.transpose(
            tensor.astype(jnp.float32).reshape(tok_rows, local_facets, LANE_DIMENSION), (1, 0, 2)
        )

    cell_out = cell_blocks(
        heads_first(queries),
        heads_first(key_rows),
        heads_first(value_rows),
        input_logits.T,
        forget_log_gate.T,
    )
    cell_out = (
        cell_out
        * rms_scale(cell_out)
        * facet_rescale_factor.reshape(local_facets, 1, LANE_DIMENSION)
    )
    cell_out = jnp.transpose(cell_out, (1, 0, 2)).reshape(tok_rows, local_width)
    slots = lax.all_to_all(outgoing_rows, "st", split_axis=0, concat_axis=0, tiled=True)
    facet_scales = lax.dynamic_slice_in_dim(affinity_scaling, first_facet, local_facets, 0)
    return attend(
        slot_index, slots, probe_vectors, mix_logits, cell_out, facet_scales, block_count
    )


def solution(mesh):
    return jax.shard_map(
        local,
        mesh=mesh,
        in_specs=(
            P("st", "tp"),
            P("st", None, None),
            P("st", None),
            P(None, "tp"),
            P(None, "tp"),
            P(None, "tp"),
            P(),
            P(),
            P("st", None),
            P("tp"),
            P(None, "tp"),
            P(None, "tp"),
            P(None, "tp"),
            P(),
            P(),
            P(None, "tp"),
        ),
        out_specs=P("st", "tp"),
        check_vma=False,
    )
```
